32 devices in a mesh: sp: 8 (over z, core), tp: 4 (over y, x).
Axes of the slice: x: 2, y: 2, z: 4, core: 2. Of those that a mesh axis runs over, the one named last changes fastest.
Arguments:
- tokens: bfloat16 [2048, 1024], P('sp', 'tp'), may hold values from -6 to 6
- norm_gain: bfloat16 [2, 1024], P(None, 'tp'), may hold values from 0.099609375 to 1.8984375
- query_weight: bfloat16 [2, 1024, 1024], P(None, 'sp', 'tp'), may hold values from -0.1875 to 0.1875
- key_weight: bfloat16 [2, 1024, 1024], P(None, 'sp', 'tp'), may hold values from -0.1875 to 0.1875
- value_weight: bfloat16 [2, 1024, 1024], P(None, 'sp', 'tp'), may hold values from -0.1875 to 0.1875
- output_weight: bfloat16 [2, 1024, 1024], P(None, 'tp', 'sp'), may hold values from -0.5 to 0.5
- offset_bias: float32 [2, 16, 15, 31], P(None, 'tp'), may hold values from -4 to 4
Outputs:
- mixed: bfloat16 [2048, 1024], P('sp', 'tp')
The draws below stay inside these ranges and needn't reach their ends.
All inputs are finite; a program needn't handle non-finite values.
Results may differ from the reference program's by a relative error of at most 0.03.
Values may be sent and summed in bfloat16 or wider, within the bound.
A program may use at most 64 MiB of HBM per device.

```python
import jax
import jax.numpy as jnp
from jax import lax

HEADS = 16
HEAD_DIM = 64
WIN_H = 8
WIN_W = 16
LAYERS = 2
COLS = 64
D = 1024
NROWS = 32
TOKENS = 2048


def levels(key, dims, shards, smallest, top_value):
    factor_of, own = 1.0, jax.random.fold_in(key, 6)
    for position, parts in shards:
        heights = jnp.exp(jax.random.uniform(jax.random.fold_in(own, position), (parts,), jnp.float32, smallest / len(shards), top_value / len(shards)))
        factor_of = factor_of * jnp.repeat(heights, dims[position] // parts).reshape([-1 if axis == position else 1 for axis in range(len(dims))])
    return factor_of


def centred(stream_key, dims, width, limit, cuts=(), held_as=jnp.bfloat16):
    values = jax.random.normal(stream_key, dims, jnp.float32) * width
    if len(cuts) > 0:
        values = levels(stream_key, dims, cuts, -0.22, 0.18) * values
    return jnp.clip(values, min=-limit, max=limit).astype(held_as)


def setup_inputs(seed: int = 0) -> dict:
    splits = jax.random.split(jax.random.key(seed), 8)
    return {
        "tokens": centred(splits[0], (TOKENS, D), 1.0, 6.0, ((0, 8), (1, 4))),
        "norm_gain": jnp.clip(1.0 + 0.18 * jax.random.normal(splits[1], (LAYERS, D), jnp.float32), 0.099609375, 1.8984375).astype(jnp.bfloat16),
        "query_weight": centred(splits[2], (LAYERS, D, D), D ** -0.5, 0.1875, ((1, 8), (2, 4))),
        "key_weight": centred(splits[3], (LAYERS, D, D), D ** -0.5, 0.1875, ((1, 8), (2, 4))),
        "value_weight": centred(splits[4], (LAYERS, D, D), D ** -0.5, 0.1875, ((1, 8), (2, 4))),
        "output_weight": centred(splits[5], (LAYERS, D, D), (D // 8) ** -0.5, 0.5, ((1, 4), (2, 8))),
        "offset_bias": centred(splits[6], (LAYERS, HEADS, 2 * WIN_H - 1, 2 * WIN_W - 1), 1.0, 4.0, ((1, 4),), jnp.float32),
    }


norm_eps = 1e-06

def neighbourhood(query, keys, values, table):
    column = jnp.arange(COLS, dtype=jnp.int32)
    col_start = jnp.clip(column - WIN_W // 2, 0, COLS - WIN_W).astype(jnp.int32)
    col_index = (col_start[:, None] + jnp.arange(WIN_W, dtype=jnp.int32)[None, :]).astype(jnp.int32)
    col_offset = (col_index - column[:, None] + (WIN_W - 1)).astype(jnp.int32)
    scale = HEAD_DIM ** (-0.5)

    def one_row(row):
        first = jnp.clip(row - WIN_H // 2, 0, NROWS - WIN_H).astype(jnp.int32)
        key_rows = lax.dynamic_slice_in_dim(keys, first, WIN_H, 0)
        value_rows = lax.dynamic_slice_in_dim(values, first, WIN_H, 0)
        key_window = key_rows[:, col_index]
        value_window = value_rows[:, col_index]
        query_row = lax.dynamic_index_in_dim(query, row, 0, keepdims=False)
        score = jnp.einsum('qhd,iqjhd->hqij', query_row.astype(jnp.float32), key_window.astype(jnp.float32)) * scale
        row_offset = first + jnp.arange(WIN_H, dtype=jnp.int32) - row + (WIN_H - 1)
        bias = table[:, row_offset[:, None, None], col_offset[None, :, :]]
        score = score + jnp.transpose(bias, (0, 2, 1, 3))
        flat = score.reshape(HEADS, COLS, WIN_H * WIN_W)
        weights = jax.nn.softmax(flat, axis=-1).reshape(score.shape).astype(jnp.bfloat16)
        out = jnp.einsum('hqij,iqjhd->qhd', weights.astype(jnp.float32), value_window.astype(jnp.float32))
        return out.astype(jnp.bfloat16)
    result = lax.map(one_row, jnp.arange(NROWS, dtype=jnp.int32))
    return result.reshape(TOKENS, D)

def reference(tokens, norm_gain, query_weight, key_weight, value_weight, output_weight, offset_bias):
    current = tokens
    for layer in range(LAYERS):
        floats = current.astype(jnp.float32)
        factor = lax.rsqrt(lax.optimization_barrier(jnp.mean(floats * floats, axis=1, keepdims=True)) + norm_eps)
        normed = (floats * factor * norm_gain[layer].astype(jnp.float32)).astype(jnp.bfloat16)
        query = jnp.dot(normed, query_weight[layer], preferred_element_type=jnp.float32).astype(jnp.bfloat16)
        keys = jnp.dot(normed, key_weight[layer], preferred_element_type=jnp.float32).astype(jnp.bfloat16)
        values = jnp.dot(normed, value_weight[layer], preferred_element_type=jnp.float32).astype(jnp.bfloat16)
        grid_shape = (NROWS, COLS, HEADS, HEAD_DIM)
        attended = neighbourhood(query.reshape(grid_shape), keys.reshape(grid_shape), values.reshape(grid_shape), offset_bias[layer].astype(jnp.float32))
        current = jnp.dot(attended, output_weight[layer], preferred_element_type=jnp.float32).astype(jnp.bfloat16)
    return current
```

```python
import functools

import jax
import jax.numpy as jnp
from jax import lax
from jax.experimental import pallas as pl
from jax.experimental.pallas import tpu as pltpu
from jax.sharding import PartitionSpec as P

MESH = pl.DeviceIdType.MESH

HEAD_DIM = 64
WIN_H = 8
WIN_W = 16
ROWS_DEV = 4
COLS = 64
D = 1024


norm_eps = 1e-06


def greet(me, n):
    barrier = pltpu.get_barrier_semaphore()
    for k in range(1, n):
        pl.semaphore_signal(
            barrier, inc=1, device_id={"tp": lax.rem(me + k, n)}, device_id_type=MESH
        )
    pl.semaphore_wait(barrier, n - 1)


def norm_kernel(n, x_ref, gain_ref, out_ref, held, gains, send, recv, gain_send, gain_recv):
    me = lax.axis_index("tp")
    width = x_ref.shape[1]
    greet(me, n)
    copies = []
    for k in range(1, n):
        peer = {"tp": lax.rem(me + k, n)}
        copies.append((
            pltpu.make_async_remote_copy(
                src_ref=x_ref, dst_ref=held.at[k - 1], send_sem=send.at[k - 1],
                recv_sem=recv.at[k - 1], device_id=peer, device_id_type=MESH,
            ),
            pltpu.make_async_remote_copy(
                src_ref=gain_ref, dst_ref=gains.at[k - 1], send_sem=gain_send.at[k - 1],
                recv_sem=gain_recv.at[k - 1], device_id=peer, device_id_type=MESH,
            ),
        ))
    for big, small in copies:
        big.start()
        small.start()
    own = x_ref[...].astype(jnp.float32)
    squares = jnp.sum(own * own, axis=1, keepdims=True)
    for k, (big, small) in enumerate(copies):
        big.wait()
        small.wait()
        part = held[k].astype(jnp.float32)
        squares = squares + jnp.sum(part * part, axis=1, keepdims=True)
    factor = lax.rsqrt(squares / (n * width) + norm_eps)
    for k in range(n):
        block = x_ref[...] if k == 0 else held[k - 1]
        gain = gain_ref[...] if k == 0 else gains[k - 1]
        scaled = block.astype(jnp.float32) * factor * gain[0:1].astype(jnp.float32)
        source = lax.rem(me - k + n, n)
        if len(out_ref.shape) == 2:
            columns = pl.ds(pl.multiple_of(source * width, width), width)
            out_ref[:, columns] = scaled.astype(jnp.bfloat16)
        else:
            out_ref[source] = scaled.astype(jnp.bfloat16)


def gathered_norm(current, gain, n, ident):
    count, width = current.shape
    wide = jnp.broadcast_to(gain[None, :], (16, width))
    flat = width % 128 == 0
    shape = (count, n * width) if flat else (n, count, width)
    vmem = pl.BlockSpec(memory_space=pltpu.VMEM)
    out = pl.pallas_call(
        functools.partial(norm_kernel, n),
        out_shape=jax.ShapeDtypeStruct(shape, jnp.bfloat16),
        in_specs=[vmem] * 2,
        out_specs=vmem,
        scratch_shapes=[
            pltpu.VMEM((n - 1, count, width), jnp.bfloat16),
            pltpu.VMEM((n - 1, 16, width), jnp.bfloat16),
        ] + [pltpu.SemaphoreType.DMA((n - 1,))] * 4,
        compiler_params=pltpu.CompilerParams(collective_id=ident, has_side_effects=True),
    )(current, wide)
    return out if flat else out.transpose(1, 0, 2).reshape(count, n * width)


def sum_kernel(n, x_ref, w_ref, out_ref, parts, held, send, recv):
    me = lax.axis_index("tp")
    width = out_ref.shape[1]
    for j in range(n):
        parts[j] = jnp.dot(
            x_ref[...], w_ref[:, j * width:(j + 1) * width], preferred_element_type=jnp.float32
        ).astype(jnp.bfloat16)
    greet(me, n)
    copies = []
    for k in range(1, n):
        peer = lax.rem(me + k, n)
        copies.append(pltpu.make_async_remote_copy(
            src_ref=parts.at[peer], dst_ref=held.at[k - 1], send_sem=send.at[k - 1],
            recv_sem=recv.at[k - 1], device_id={"tp": peer}, device_id_type=MESH,
        ))
    for copy in copies:
        copy.start()
    total = parts[me].astype(jnp.float32)
    for k, copy in enumerate(copies):
        copy.wait()
        total = total + held[k].astype(jnp.float32)
    out_ref[...] = total.astype(jnp.bfloat16)


def projected_sum(attended, weight, n, ident):
    count = attended.shape[0]
    width = weight.shape[1] // n
    vmem = pl.BlockSpec(memory_space=pltpu.VMEM)
    return pl.pallas_call(
        functools.partial(sum_kernel, n),
        out_shape=jax.ShapeDtypeStruct((count, width), jnp.bfloat16),
        in_specs=[vmem] * 2,
        out_specs=vmem,
        scratch_shapes=[
            pltpu.VMEM((n, count, width), jnp.bfloat16),
            pltpu.VMEM((n - 1, count, width), jnp.bfloat16),
        ] + [pltpu.SemaphoreType.DMA((n - 1,))] * 2,
        compiler_params=pltpu.CompilerParams(collective_id=ident, has_side_effects=True),
    )(attended, weight)


def extended(block, sides, width, periodic):
    for axis, dim in sides:
        count = lax.axis_size(axis)
        forward = [(i, i + 1) for i in range(count - 1)]
        if periodic:
            forward.append((count - 1, 0))
        backward = [(target, source) for source, target in forward]
        low = lax.ppermute(
            lax.slice_in_dim(block, block.shape[dim] - width, None, axis=dim), axis, forward
        )
        high = lax.ppermute(lax.slice_in_dim(block, 0, width, axis=dim), axis, backward)
        block = jnp.concatenate([low, block, high], axis=dim)
    return block


def attend(query, padded, table, base, total_rows):
    heads = table.shape[0]
    local_width = heads * HEAD_DIM
    half = WIN_H // 2
    span_rows = ROWS_DEV + WIN_H
    glob = base + jnp.arange(ROWS_DEV, dtype=jnp.int32)
    first = jnp.clip(glob - half, 0, total_rows - WIN_H).astype(jnp.int32)
    local_first = first - base + half
    padded_row = jnp.arange(span_rows, dtype=jnp.int32)
    row_inside = (padded_row[None, :] >= local_first[:, None]) & (
        padded_row[None, :] < local_first[:, None] + WIN_H
    )
    row_offset = padded_row[None, :] + base - half - glob[:, None] + (WIN_H - 1)
    row_codes = jnp.arange(2 * WIN_H - 1, dtype=jnp.int32)
    row_onehot = (row_offset[:, :, None] == row_codes[None, None, :]).astype(jnp.float32)
    column = jnp.arange(COLS, dtype=jnp.int32)
    col_start = jnp.clip(column - WIN_W // 2, 0, COLS - WIN_W).astype(jnp.int32)
    col_inside = (column[None, :] >= col_start[:, None]) & (
        column[None, :] < col_start[:, None] + WIN_W
    )
    col_offset = column[None, :] - column[:, None] + (WIN_W - 1)
    col_codes = jnp.arange(2 * WIN_W - 1, dtype=jnp.int32)
    col_onehot = (col_offset[:, :, None] == col_codes[None, None, :]).astype(jnp.float32)
    bias = jnp.einsum(
        "hab,ria,qkb->rhqik", table, row_onehot, col_onehot, precision=lax.Precision.HIGHEST
    )
    inside = row_inside[:, None, None, :, None] & col_inside[None, None, :, None, :]
    keys = padded[:, :, :local_width].reshape(span_rows, COLS, heads, HEAD_DIM)
    values = padded[:, :, local_width:].reshape(span_rows, COLS, heads, HEAD_DIM)
    grid_query = query.reshape(ROWS_DEV, COLS, heads, HEAD_DIM)
    score = jnp.einsum(
        "rqhd,ikhd->rhqik", grid_query, keys, preferred_element_type=jnp.float32
    ) * HEAD_DIM ** (-0.5)
    score = jnp.where(inside, score + bias, -1e30)
    flat = score.reshape(ROWS_DEV, heads, COLS, span_rows * COLS)
    weights = jax.nn.softmax(flat, axis=-1).reshape(score.shape).astype(jnp.bfloat16)
    out = jnp.einsum(
        "rhqik,ikhd->rqhd", weights, values, preferred_element_type=jnp.float32
    ).astype(jnp.bfloat16)
    return out.reshape(ROWS_DEV * COLS, local_width)


def body(tokens, norm_gain, query_weight, key_weight, value_weight, output_weight, offset_bias):
    layers = query_weight.shape[0]
    local_width = query_weight.shape[2]
    n = lax.axis_size("tp")
    half = WIN_H // 2
    base = lax.axis_index("sp") * ROWS_DEV
    total_rows = ROWS_DEV * lax.axis_size("sp")
    current = tokens
    every = []
    for layer in range(layers):
        own = jnp.concatenate(
            [query_weight[layer], key_weight[layer], value_weight[layer]], axis=1
        )
        every.append((
            lax.all_gather(own, "sp", axis=0, tiled=True),
            lax.all_gather(output_weight[layer], "sp", axis=1, tiled=True),
        ))
    for layer in range(layers):
        stacked, output_full = every[layer]
        normed = gathered_norm(current, norm_gain[layer], n, 2 * layer)
        table = offset_bias[layer].astype(jnp.float32)
        projected = jnp.dot(normed, stacked, preferred_element_type=jnp.float32).astype(
            jnp.bfloat16
        )
        query = projected[:, :local_width]
        pair = projected[:, local_width:].reshape(ROWS_DEV, COLS, 2 * local_width)
        padded = extended(pair, (("sp", 0),), half, False)
        attended = attend(query, padded, table, base, total_rows)
        current = projected_sum(attended, output_full, n, 2 * layer + 1)
    return current


def solution(mesh):
    in_specs = (
        P("sp", "tp"),
        P(None, "tp"),
        P(None, "sp", "tp"),
        P(None, "sp", "tp"),
        P(None, "sp", "tp"),
        P(None, "tp", "sp"),
        P(None, "tp", None, None),
    )
    out_specs = P("sp", "tp")
    return jax.shard_map(body, mesh=mesh, in_specs=in_specs, out_specs=out_specs, check_vma=False)
```
